32 devices in a mesh: grp: 2 (over y), sp: 4 (over z), tp: 4 (over x, core).
Axes of the slice: x: 2, y: 2, z: 4, core: 2. Of those that a mesh axis runs over, the one named last changes fastest.
Arguments:
- tokens: bfloat16 [6144, 2048], P(('grp', 'sp'), 'tp'), parts along dimension 0, may hold values from -8 to 8
- norm_gain: float32 [2, 2048], replicated, may hold values from 0.1 to 1.9
- w_value: bfloat16 [2, 2048, 2048], P(None, 'sp', 'tp'), may hold values from -0.125 to 0.125
- w_gate: bfloat16 [2, 2048, 2048], P(None, 'sp', 'tp'), may hold values from -0.125 to 0.125
- taps: float32 [2, 31, 2048], P(None, None, 'tp'), may hold values from -2 to 2
- ln_gain: float32 [2, 2048], P(None, 'tp'), may hold values from 0.1 to 1.9
- ln_shift: float32 [2, 2048], P(None, 'tp'), may hold values from -3 to 3
- w_out: bfloat16 [2, 2048, 2048], P(None, 'sp', 'tp'), may hold values from -0.125 to 0.125
Outputs:
- stream_out: bfloat16 [6144, 2048], P(('grp', 'sp'), 'tp'), parts along dimension 0
The draws below stay inside these ranges and needn't reach their ends.
There are 2 independent parts, one for each index of `grp`. The reference program is written for one: setup_inputs(seed, part) draws one part's arguments, and reference() takes and returns one part's arrays. A program takes and returns all parts, laid end to end along the dimension named above; an argument that names none is the same for every part. Nothing has to cross between parts.
All inputs are finite; a program needn't handle non-finite values.
Results may differ from the reference program's by a relative error of at most 0.012.
Values may be sent and summed in bfloat16 or wider, within the bound.
A program may use at most 64 MiB of HBM per device.

```python
import jax
import jax.numpy as jnp
from jax import lax

D = 2048
C = 2048
KERNEL = 31
LAYERS = 2
TOKENS = 3072


def draw_tokens(key, part):
    first, second = jax.random.split(jax.random.fold_in(key, 11), 2)
    ramp = jnp.exp(jnp.linspace(-0.7, 0.7, D))
    rough = jnp.exp(jax.random.uniform(second, (D,), minval=-0.5, maxval=0.5))
    base = jnp.clip(jax.random.normal(first, (TOKENS, D)), -2.4, 2.4)
    return (base * ramp * rough).astype(jnp.bfloat16)


def draw_taps(key, part):
    first, second = jax.random.split(jax.random.fold_in(key, 23), 2)
    ramp = jnp.exp(jnp.linspace(-0.7, 0.7, C))
    rough = jnp.exp(jax.random.uniform(second, (C,), minval=-0.4, maxval=0.4))
    base = jnp.clip(jax.random.normal(first, (LAYERS, KERNEL, C)), -3.0, 3.0)
    return (base * KERNEL ** (-0.5) * ramp * rough).astype(jnp.float32)


def block_scale(stream_key, dims, cuts, smallest, top_value):
    def one(dim, blocks):
        draws = jax.random.uniform(jax.random.fold_in(jax.random.fold_in(stream_key, 6), dim), (blocks,), jnp.float32, smallest / len(cuts), top_value / len(cuts))
        return jnp.repeat(jnp.exp(draws), dims[dim] // blocks).reshape((-1,) + (1,) * (len(dims) - dim - 1))

    factor_of = one(*cuts[0])
    for cut in cuts[1:]:
        factor_of = factor_of * one(*cut)
    return factor_of


def normal_values(stream_key, shape, deviation, most, shards=(), dtype=jnp.bfloat16):
    array = deviation * jax.random.normal(stream_key, shape, jnp.float32)
    if shards:
        array = array * block_scale(stream_key, shape, shards, -0.22, 0.18)
    return jnp.clip(array, -most, most).astype(dtype)


def setup_inputs(seed: int = 0, part: int = 0) -> dict:
    keys = jax.random.split(jax.random.key(seed), 9)
    part_keys = jax.random.split(jax.random.fold_in(keys[8], part), 9)
    tokens = draw_tokens(jax.random.fold_in(jax.random.fold_in(keys[8], part), 71), part)
    norm_gain = jnp.clip(1.0 + 0.18 * jax.random.normal(keys[1], (LAYERS, D), jnp.float32), 0.1, 1.9)
    w_value = normal_values(keys[2], (LAYERS, D, C), D ** -0.5, 0.125, ((1, 4), (2, 4)))
    w_gate = normal_values(keys[3], (LAYERS, D, C), D ** -0.5, 0.125, ((1, 4), (2, 4)))
    taps = draw_taps(jax.random.fold_in(keys[8], 71), part)
    ln_gain = jnp.clip(1.0 + 0.18 * jax.random.normal(keys[5], (LAYERS, C), jnp.float32), 0.1, 1.9)
    ln_shift = normal_values(keys[6], (LAYERS, C), 0.5, 3.0, ((1, 4),), jnp.float32)
    w_out = normal_values(keys[7], (LAYERS, C, D), C ** -0.5, 0.125, ((1, 4), (2, 4)))
    return {"tokens": tokens, "norm_gain": norm_gain, "w_value": w_value, "w_gate": w_gate, "taps": taps, "ln_gain": ln_gain, "ln_shift": ln_shift, "w_out": w_out}


def reference(tokens, norm_gain, w_value, w_gate, taps, ln_gain, ln_shift, w_out):
    half = (KERNEL - 1) // 2
    stream = tokens
    for layer in range(LAYERS):
        wide = stream.astype(jnp.float32)
        meansq = lax.optimization_barrier(jnp.mean(wide * wide, axis=1, keepdims=True))
        normed = (wide * lax.rsqrt(meansq + 1e-06) * norm_gain[layer]).astype(jnp.bfloat16)
        value = jnp.dot(normed, w_value[layer], preferred_element_type=jnp.float32)
        gate = jnp.dot(normed, w_gate[layer], preferred_element_type=jnp.float32)
        glu = (value * jax.nn.sigmoid(gate)).astype(jnp.bfloat16)
        padded = jnp.pad(glu.astype(jnp.float32), ((half, half), (0, 0)))
        count = glu.shape[0]
        conv = jnp.zeros(glu.shape, jnp.float32)
        for step in range(KERNEL):
            conv = conv + taps[layer, step][None, :] * padded[step:step + count]
        mean_c = lax.optimization_barrier(jnp.mean(conv, axis=1, keepdims=True))
        var_c = lax.optimization_barrier(jnp.mean(conv * conv, axis=1, keepdims=True)) - mean_c * mean_c
        shaped = (conv - mean_c) * lax.rsqrt(var_c + 1e-05) * ln_gain[layer] + ln_shift[layer]
        act = jax.nn.silu(shaped).astype(jnp.bfloat16)
        update = jnp.dot(act, w_out[layer], preferred_element_type=jnp.float32)
        stream = (stream.astype(jnp.float32) + update).astype(jnp.bfloat16)
    return stream
```

```python
import functools

import jax
import jax.numpy as jnp
from jax import lax
from jax.experimental import pallas as pl
from jax.experimental.pallas import tpu as pltpu
from jax.sharding import PartitionSpec as P

MESH = pl.DeviceIdType.MESH
HALO = 16
LANES = 128
BLOCK = 64


def body(
    sizes,
    tokens,
    norm_gain,
    w_value,
    w_gate,
    taps,
    ln_gain,
    ln_shift,
    w_out,
    out,
    weights,
    gathered,
    glu,
    conv,
    stats,
    load_sem,
    z_send,
    z_recv,
    y_send,
    y_recv,
    x_send,
    x_recv,
    s_send,
    s_recv,
    h_send,
    h_recv,
):
    groups, n, tp, chunks, subs = sizes
    chips = tp // 2
    grp, sp, me = lax.axis_index("grp"), lax.axis_index("sp"), lax.axis_index("tp")
    chip, core = me // 2, me % 2
    partner = chip * 2 + 1 - core
    layers, depth, cols = w_value.shape
    kernel = taps.shape[1]
    half = (kernel - 1) // 2
    count = tokens.shape[0]
    rows = count // chunks
    width = cols * tp
    pieces = layers * 3 * subs
    part = depth // (groups * subs)
    hops = n - 1
    per_matrix = subs * hops
    f32, bf16 = jnp.float32, jnp.bfloat16

    def aligned(value, unit):
        return pl.multiple_of(value, unit)

    barrier = pltpu.get_barrier_semaphore()
    for off in range(1, tp):
        pl.semaphore_signal(
            barrier, inc=1, device_id={"tp": (me + off) % tp}, device_id_type=MESH
        )
    for off in range(1, groups):
        pl.semaphore_signal(
            barrier, inc=1, device_id={"grp": (grp + off) % groups}, device_id_type=MESH
        )

    @pl.when(sp > 0)
    def _():
        pl.semaphore_signal(barrier, inc=1, device_id={"sp": sp - 1}, device_id_type=MESH)

    @pl.when(sp < n - 1)
    def _():
        pl.semaphore_signal(barrier, inc=1, device_id={"sp": sp + 1}, device_id_type=MESH)

    def own_load(matrix):
        source = (w_value, w_gate, w_out)[matrix % 3]
        return pltpu.make_async_copy(
            source.at[matrix // 3],
            weights.at[matrix, pl.ds(aligned(sp * depth, 16), depth), :],
            load_sem.at[matrix],
        )

    for matrix in range(layers * 3):
        own_load(matrix).start()

    def piece(block, m, quarter):
        start = block * depth + ((m % subs) * groups + quarter) * part
        return weights.at[m // subs, pl.ds(aligned(start, 16), part), :]

    def z_copy(way, m, hop, block):
        ref = piece(block, m, grp)
        return pltpu.make_async_remote_copy(
            src_ref=ref,
            dst_ref=ref,
            send_sem=z_send.at[way, m, hop],
            recv_sem=z_recv.at[way, m, hop],
            device_id={"sp": sp + 1 if way == 0 else sp - 1},
            device_id_type=MESH,
        )

    def y_copy(m, block, off, quarter):
        ref = piece(block, m, quarter)
        return pltpu.make_async_remote_copy(
            src_ref=ref,
            dst_ref=ref,
            send_sem=y_send.at[m, block, off - 1],
            recv_sem=y_recv.at[m, block, off - 1],
            device_id={"grp": (grp + off) % groups},
            device_id_type=MESH,
        )

    def send_own(m):
        @pl.when(sp < n - 1)
        def _():
            z_copy(0, m, 0, sp).start()

        @pl.when(sp > 0)
        def _():
            z_copy(1, m, 0, sp).start()

    def weight_step(k):
        m, r = k // hops, k % hops

        @pl.when(sp - (r + 1) >= 0)
        def _():
            block = sp - (r + 1)
            z_copy(0, m, r, block).wait_recv()

            @pl.when(sp < n - 1)
            def _():
                z_copy(0, m, r + 1, block).start()

            for off in range(1, groups):
                y_copy(m, block, off, grp).start()

        @pl.when(sp + (r + 1) < n)
        def _():
            block = sp + (r + 1)
            z_copy(1, m, r, block).wait_recv()

            @pl.when(sp > 0)
            def _():
                z_copy(1, m, r + 1, block).start()

            for off in range(1, groups):
                y_copy(m, block, off, grp).start()

        @pl.when(jnp.logical_and(r == hops - 1, m + 2 < pieces))
        def _():
            send_own(m + 2)

    def weight_steps(low, high):
        lax.fori_loop(low, high, lambda k, c: (weight_step(k), c)[1], 0)

    def weight_share(low, high, i):
        span = high - low
        weight_steps(low + span * i // chunks, low + span * (i + 1) // chunks)

    def matrix_wait(matrix):
        def wait(i, c):
            m, block = matrix * subs + i // n, i % n

            @pl.when(block != sp)
            def _():
                for off in range(1, groups):
                    y_copy(m, block, off, (grp + groups - off) % groups).wait_recv()

            return c

        lax.fori_loop(0, subs * n, wait, 0)

    def chunk_rows(c):
        return pl.ds(aligned(c * rows, rows), rows)

    def x_copy(phase, c, source, slot, target):
        ref = gathered.at[phase, chunk_rows(c), pl.ds(aligned(source * cols, LANES), cols)]
        return pltpu.make_async_remote_copy(
            src_ref=ref,
            dst_ref=ref,
            send_sem=x_send.at[phase, c, slot],
            recv_sem=x_recv.at[phase, c, source],
            device_id={"tp": target},
            device_id_type=MESH,
        )

    def x_own(phase, c):
        for off in range(1, chips):
            x_copy(phase, c, me, off - 1, ((chip + off) % chips) * 2 + core).start()
        x_copy(phase, c, me, chips - 1, partner).start()

    def x_forward(phase, c):
        for off in range(1, chips):
            source = ((chip + off) % chips) * 2 + core
            x_copy(phase, c, source, 0, partner).wait_recv()
            x_copy(phase, c, source, chips - 1 + off, partner).start()

    def x_wait(phase, c):
        for off in range(chips):
            source = ((chip + off) % chips) * 2 + 1 - core
            x_copy(phase, c, source, 0, partner).wait_recv()

    def s_copy(phase, c, source, slot, target):
        ref = stats.at[phase, c, source]
        return pltpu.make_async_remote_copy(
            src_ref=ref,
            dst_ref=ref,
            send_sem=s_send.at[phase, c, slot],
            recv_sem=s_recv.at[phase, c, source],
            device_id={"tp": target},
            device_id_type=MESH,
        )

    def s_share(phase, c, first, second):
        lane = lax.broadcasted_iota(jnp.int32, (rows, LANES), 1)
        both = jnp.where(lane < 4, first, second)
        stats[phase, c, me] = both.T[:8]
        for off in range(1, tp):
            s_copy(phase, c, me, off - 1, (me + off) % tp).start()

    def s_total(phase, c):
        for off in range(1, tp):
            s_copy(phase, c, (me + off) % tp, 0, me).wait_recv()
        total = stats[phase, c, 0]
        for source in range(1, tp):
            total = total + stats[phase, c, source]
        return jnp.concatenate([total] * (LANES // 8), axis=0).T

    def h_copy(layer, way):
        if way == 0:
            source, target, device = count, 0, sp + 1
        else:
            source, target, device = HALO, HALO + count, sp - 1
        return pltpu.make_async_remote_copy(
            src_ref=glu.at[layer, pl.ds(source, HALO), :],
            dst_ref=glu.at[layer, pl.ds(target, HALO), :],
            send_sem=h_send.at[layer, way],
            recv_sem=h_recv.at[layer, way],
            device_id={"sp": device},
            device_id_type=MESH,
        )

    mine = pl.ds(aligned(me * cols, LANES), cols)

    def share_stream(layer, c, wide):
        s_share(2 * layer, c, jnp.sum(wide * wide, axis=1, keepdims=True), 0.0)
        gain = norm_gain[pl.ds(layer, 1), mine]
        gathered[2 * layer, chunk_rows(c), mine] = (wide * gain).astype(bf16)
        x_own(2 * layer, c)

    def loop(function):
        lax.fori_loop(0, chunks, lambda i, c: (function(i), c)[1], 0)

    def inner_first(i):
        return (1 + 2 * i) % chunks

    def ends_first(i):
        return (2 * i) % chunks

    for layer in range(layers):

        @pl.when(sp == 0)
        def _():
            glu[layer, pl.ds(0, HALO), :] = jnp.zeros((HALO, cols), bf16)

        @pl.when(sp == n - 1)
        def _():
            glu[layer, pl.ds(HALO + count, HALO), :] = jnp.zeros((HALO, cols), bf16)

    for matrix in range(layers * 3):
        own_load(matrix).wait()
    pl.semaphore_wait(
        barrier,
        tp - 1 + groups - 1 + (sp > 0).astype(jnp.int32) + (sp < n - 1).astype(jnp.int32),
    )
    send_own(0)
    send_own(1)

    loop(lambda c: share_stream(0, c, tokens[chunk_rows(c), :].astype(f32)))

    def gated(layer, low, high, i):
        c = ends_first(i)
        phase = 2 * layer
        scale = lax.rsqrt(s_total(phase, c)[:, :1] / width + 1e-06)
        block = gathered[phase, chunk_rows(c), :]
        value = jnp.dot(block, weights[3 * layer], preferred_element_type=f32) * scale
        gate = jnp.dot(block, weights[3 * layer + 1], preferred_element_type=f32) * scale
        glu[layer, pl.ds(aligned(HALO + c * rows, HALO), rows), :] = (
            value * jax.nn.sigmoid(gate)
        ).astype(bf16)

        @pl.when(jnp.logical_and(c == 0, sp > 0))
        def _():
            h_copy(layer, 1).start()

        @pl.when(jnp.logical_and(c == chunks - 1, sp < n - 1))
        def _():
            h_copy(layer, 0).start()

        weight_share(low, high, i)

    shift = HALO - half
    groups_of_8 = (kernel + shift + 7) // 8
    window = BLOCK + 8 * groups_of_8

    def convolve(layer, c):
        lane_blocks = cols // LANES

        def block(i, carry):
            base = aligned(c * rows + (i // lane_blocks) * BLOCK, BLOCK)
            lanes = pl.ds(aligned((i % lane_blocks) * LANES, LANES), LANES)
            values = glu[layer, pl.ds(base, window), lanes].astype(f32)
            total = None
            for j in range(8):
                partial = None
                for g in range(groups_of_8):
                    tap = 8 * g + j - shift
                    if tap < 0 or tap >= kernel:
                        continue
                    term = taps[layer, pl.ds(tap, 1), lanes] * values[8 * g : 8 * g + BLOCK + 8]
                    partial = term if partial is None else partial + term
                piece_j = partial[j : j + BLOCK]
                total = piece_j if total is None else total + piece_j
            conv[pl.ds(base, BLOCK), lanes] = total
            return carry

        lax.fori_loop(0, rows // BLOCK * lane_blocks, block, 0)

    def mixed(layer, low, high, i):
        c = inner_first(i)

        @pl.when(jnp.logical_and(c == 0, sp > 0))
        def _():
            h_copy(layer, 0).wait_recv()

        @pl.when(jnp.logical_and(c == chunks - 1, sp < n - 1))
        def _():
            h_copy(layer, 1).wait_recv()

        convolve(layer, c)
        whole = conv[chunk_rows(c), :]
        s_share(
            2 * layer + 1,
            c,
            jnp.sum(whole, axis=1, keepdims=True),
            jnp.sum(whole * whole, axis=1, keepdims=True),
        )
        weight_share(low, high, i)

    def activate(layer, i):
        c = inner_first(i)
        total = s_total(2 * layer + 1, c)
        mean = total[:, :1] / width
        var = total[:, 4:5] / width - mean * mean
        gain = ln_gain[pl.ds(layer, 1), :]
        moved = ln_shift[pl.ds(layer, 1), :]
        shaped = (conv[chunk_rows(c), :] - mean) * lax.rsqrt(var + 1e-05) * gain + moved
        act = shaped * jax.nn.sigmoid(shaped)
        gathered[2 * layer + 1, chunk_rows(c), mine] = act.astype(bf16)
        x_own(2 * layer + 1, c)

    def close(layer, low, high, i):
        c = inner_first(i)
        phase = 2 * layer + 1
        x_forward(phase, c)
        x_wait(phase, c)
        update = jnp.dot(
            gathered[phase, chunk_rows(c), :],
            weights[3 * layer + 2],
            preferred_element_type=f32,
        )
        source = tokens if layer == 0 else out
        stream = (source[chunk_rows(c), :].astype(f32) + update).astype(bf16)
        out[chunk_rows(c), :] = stream
        if layer + 1 < layers:
            share_stream(layer + 1, c, stream.astype(f32))
            weight_share(low, high, i)

    def arrive(layer, low, high, i):
        c = i if layer == 0 else inner_first(i)
        x_forward(2 * layer, c)
        x_wait(2 * layer, c)
        weight_share(low, high, i)

    for layer in range(layers):
        first = 3 * layer * per_matrix
        if layer == 0:
            loop(functools.partial(arrive, layer, first, first + 2 * per_matrix))
        else:
            loop(functools.partial(arrive, layer, first + per_matrix, first + 2 * per_matrix))
        matrix_wait(3 * layer)
        matrix_wait(3 * layer + 1)
        closing = first + 2 * per_matrix
        middle = closing + per_matrix // 2
        loop(functools.partial(gated, layer, closing, middle))
        loop(functools.partial(mixed, layer, middle, closing + per_matrix))
        loop(functools.partial(activate, layer))
        matrix_wait(3 * layer + 2)
        after = closing + per_matrix
        loop(functools.partial(close, layer, after, after + per_matrix))

    def drain_weights(i, carry):
        m, block = i // n, i % n

        @pl.when(block <= sp)
        def _():
            @pl.when(sp < n - 1)
            def _():
                z_copy(0, m, sp - block, block).wait_send()

        @pl.when(block >= sp)
        def _():
            @pl.when(sp > 0)
            def _():
                z_copy(1, m, block - sp, block).wait_send()

        @pl.when(block != sp)
        def _():
            for off in range(1, groups):
                y_copy(m, block, off, grp).wait_send()

        return carry

    lax.fori_loop(0, pieces * n, drain_weights, 0)

    def drain_chunks(i, carry):
        phase, c = i // chunks, i % chunks
        for slot in range(tp - 1):
            x_copy(phase, c, me, slot, partner).wait_send()
            s_copy(phase, c, me, slot, partner).wait_send()
        return carry

    lax.fori_loop(0, 2 * layers * chunks, drain_chunks, 0)
    for layer in range(layers):

        @pl.when(sp < n - 1)
        def _():
            h_copy(layer, 0).wait_send()

        @pl.when(sp > 0)
        def _():
            h_copy(layer, 1).wait_send()


def solution(mesh):
    groups, n, tp = mesh.shape["grp"], mesh.shape["sp"], mesh.shape["tp"]

    def shards(tokens, norm_gain, w_value, w_gate, taps, ln_gain, ln_shift, w_out):
        layers, depth, cols = w_value.shape
        count = tokens.shape[0]
        chunks = 3
        subs = 2 if depth >= 512 else 1
        pieces = layers * 3 * subs
        rows = count // chunks
        vmem = pl.BlockSpec(memory_space=pltpu.VMEM)
        hbm = pl.BlockSpec(memory_space=pl.ANY)
        dma = pltpu.SemaphoreType.DMA
        return pl.pallas_call(
            functools.partial(body, (groups, n, tp, chunks, subs)),
            out_shape=jax.ShapeDtypeStruct((count, cols), jnp.bfloat16),
            in_specs=[vmem, vmem, hbm, hbm, vmem, vmem, vmem, hbm],
            out_specs=vmem,
            scratch_shapes=[
                pltpu.VMEM((layers * 3, depth * n, cols), jnp.bfloat16),
                pltpu.VMEM((2 * layers, count, cols * tp), jnp.bfloat16),
                pltpu.VMEM((layers, count + 2 * HALO, cols), jnp.bfloat16),
                pltpu.VMEM((count, cols), jnp.float32),
                pltpu.VMEM((2 * layers, chunks, tp, 8, rows), jnp.float32),
                dma((layers * 3,)),
                dma((2, pieces, n - 1)),
                dma((2, pieces, n - 1)),
                dma((pieces, n, groups - 1)),
                dma((pieces, n, groups - 1)),
                dma((2 * layers, chunks, tp - 1)),
                dma((2 * layers, chunks, tp)),
                dma((2 * layers, chunks, tp - 1)),
                dma((2 * layers, chunks, tp)),
                dma((layers, 2)),
                dma((layers, 2)),
            ],
            compiler_params=pltpu.CompilerParams(
                collective_id=0, has_side_effects=True, vmem_limit_bytes=60 * 1024 * 1024
            ),
        )(tokens, norm_gain, w_value, w_gate, taps, ln_gain, ln_shift, w_out)

    return jax.shard_map(
        shards,
        mesh=mesh,
        in_specs=(
            P(("grp", "sp"), "tp"),
            P(),
            P(None, "sp", "tp"),
            P(None, "sp", "tp"),
            P(None, None, "tp"),
            P(None, "tp"),
            P(None, "tp"),
            P(None, "sp", "tp"),
        ),
        out_specs=P(("grp", "sp"), "tp"),
        check_vma=False,
    )
```

```python
import functools

import jax
import jax.numpy as jnp
from jax import lax
from jax.experimental import pallas as pl
from jax.experimental.pallas import tpu as pltpu
from jax.sharding import PartitionSpec as P

MESH = pl.DeviceIdType.MESH
HALO = 16
LANES = 128
BLOCK = 64
LEAD = 4


def body(
    sizes,
    tokens,
    norm_gain,
    w_value,
    w_gate,
    taps_in,
    ln_gain,
    ln_shift,
    w_out,
    out,
    taps,
    weights,
    gathered,
    glu,
    conv,
    stats,
    load_sem,
    z_send,
    z_recv,
    y_send,
    y_recv,
    x_send,
    x_recv,
    s_send,
    s_recv,
    h_send,
    h_recv,
):
    groups, n, tp, chunks, subs, ahead = sizes
    chips = tp // 2
    grp, sp, me = lax.axis_index("grp"), lax.axis_index("sp"), lax.axis_index("tp")
    chip, core = me // 2, me % 2
    partner = chip * 2 + 1 - core
    layers, depth, cols = w_value.shape
    kernel = taps_in.shape[1]
    half = (kernel - 1) // 2
    count = tokens.shape[0]
    rows = count // chunks
    width = cols * tp
    pieces = layers * 3 * subs
    part = depth // (groups * subs)
    hops = n - 1
    per_matrix = subs * hops
    lead = LEAD
    f32, bf16 = jnp.float32, jnp.bfloat16

    def aligned(value, unit):
        return pl.multiple_of(value, unit)

    barrier = pltpu.get_barrier_semaphore()
    for off in range(1, tp):
        pl.semaphore_signal(
            barrier, inc=1, device_id={"tp": (me + off) % tp}, device_id_type=MESH
        )
    for off in range(1, groups):
        pl.semaphore_signal(
            barrier, inc=1, device_id={"grp": (grp + off) % groups}, device_id_type=MESH
        )

    @pl.when(sp > 0)
    def _():
        pl.semaphore_signal(barrier, inc=1, device_id={"sp": sp - 1}, device_id_type=MESH)

    @pl.when(sp < n - 1)
    def _():
        pl.semaphore_signal(barrier, inc=1, device_id={"sp": sp + 1}, device_id_type=MESH)

    def own_load(matrix):
        source = (w_value, w_gate, w_out)[matrix % 3]
        return pltpu.make_async_copy(
            source.at[matrix // 3],
            weights.at[matrix, pl.ds(aligned(sp * depth, 16), depth), :],
            load_sem.at[matrix],
        )

    taps_load = pltpu.make_async_copy(taps_in, taps, load_sem.at[layers * 3])
    for matrix in range(layers * 3):
        own_load(matrix).start()
    taps_load.start()

    def piece(block, m, quarter):
        start = block * depth + ((m % subs) * groups + quarter) * part
        return weights.at[m // subs, pl.ds(aligned(start, 16), part), :]

    def z_copy(way, m, hop, block):
        ref = piece(block, m, grp)
        return pltpu.make_async_remote_copy(
            src_ref=ref,
            dst_ref=ref,
            send_sem=z_send.at[way, m, hop],
            recv_sem=z_recv.at[way, m, hop],
            device_id={"sp": sp + 1 if way == 0 else sp - 1},
            device_id_type=MESH,
        )

    def y_copy(m, block, off, quarter):
        ref = piece(block, m, quarter)
        return pltpu.make_async_remote_copy(
            src_ref=ref,
            dst_ref=ref,
            send_sem=y_send.at[m, block, off - 1],
            recv_sem=y_recv.at[m, block, off - 1],
            device_id={"grp": (grp + off) % groups},
            device_id_type=MESH,
        )

    def send_own(m):
        @pl.when(sp < n - 1)
        def _():
            z_copy(0, m, 0, sp).start()

        @pl.when(sp > 0)
        def _():
            z_copy(1, m, 0, sp).start()

    def weight_step(k):
        m, r = k // hops, k % hops

        @pl.when(sp - (r + 1) >= 0)
        def _():
            block = sp - (r + 1)
            z_copy(0, m, r, block).wait_recv()

            @pl.when(sp < n - 1)
            def _():
                z_copy(0, m, r + 1, block).start()

            for off in range(1, groups):
                y_copy(m, block, off, grp).start()

        @pl.when(sp + (r + 1) < n)
        def _():
            block = sp + (r + 1)
            z_copy(1, m, r, block).wait_recv()

            @pl.when(sp > 0)
            def _():
                z_copy(1, m, r + 1, block).start()

            for off in range(1, groups):
                y_copy(m, block, off, grp).start()

        @pl.when(jnp.logical_and(r == hops - 1, m + ahead < pieces))
        def _():
            send_own(m + ahead)

    def weight_steps(low, high):
        lax.fori_loop(low, high, lambda k, c: (weight_step(k), c)[1], 0)

    def weight_share(low, high, i):
        span = high - low
        weight_steps(low + span * i // chunks, low + span * (i + 1) // chunks)

    def matrix_wait(matrix):
        def wait(i, c):
            m, block = matrix * subs + i // n, i % n

            @pl.when(block != sp)
            def _():
                for off in range(1, groups):
                    y_copy(m, block, off, (grp + groups - off) % groups).wait_recv()

            return c

        lax.fori_loop(0, subs * n, wait, 0)

    def chunk_rows(c):
        return pl.ds(aligned(c * rows, rows), rows)

    def x_copy(phase, c, source, slot, target):
        ref = gathered.at[phase, chunk_rows(c), pl.ds(aligned(source * cols, LANES), cols)]
        return pltpu.make_async_remote_copy(
            src_ref=ref,
            dst_ref=ref,
            send_sem=x_send.at[phase, c, slot],
            recv_sem=x_recv.at[phase, c, source],
            device_id={"tp": target},
            device_id_type=MESH,
        )

    def x_own(phase, c):
        for off in range(1, chips):
            x_copy(phase, c, me, off - 1, ((chip + off) % chips) * 2 + core).start()
        x_copy(phase, c, me, chips - 1, partner).start()

    def x_forward(phase, c):
        for off in range(1, chips):
            source = ((chip + off) % chips) * 2 + core
            x_copy(phase, c, source, 0, partner).wait_recv()
            x_copy(phase, c, source, chips - 1 + off, partner).start()

    def x_wait(phase, c):
        for off in range(chips):
            source = ((chip + off) % chips) * 2 + 1 - core
            x_copy(phase, c, source, 0, partner).wait_recv()

    def s_copy(phase, c, source, slot, target):
        ref = stats.at[phase, c, source]
        return pltpu.make_async_remote_copy(
            src_ref=ref,
            dst_ref=ref,
            send_sem=s_send.at[phase, c, slot],
            recv_sem=s_recv.at[phase, c, source],
            device_id={"tp": target},
            device_id_type=MESH,
        )

    def s_share(phase, c, first, second):
        lane = lax.broadcasted_iota(jnp.int32, (rows, LANES), 1)
        both = jnp.where(lane < 4, first, second)
        stats[phase, c, me] = both.T[:8]
        for off in range(1, tp):
            s_copy(phase, c, me, off - 1, (me + off) % tp).start()

    def s_total(phase, c):
        for off in range(1, tp):
            s_copy(phase, c, (me + off) % tp, 0, me).wait_recv()
        total = stats[phase, c, 0]
        for source in range(1, tp):
            total = total + stats[phase, c, source]
        return jnp.concatenate([total] * (LANES // 8), axis=0).T

    def h_copy(layer, way):
        if way == 0:
            source, target, device = count, 0, sp + 1
        else:
            source, target, device = HALO, HALO + count, sp - 1
        return pltpu.make_async_remote_copy(
            src_ref=glu.at[layer, pl.ds(source, HALO), :],
            dst_ref=glu.at[layer, pl.ds(target, HALO), :],
            send_sem=h_send.at[layer, way],
            recv_sem=h_recv.at[layer, way],
            device_id={"sp": device},
            device_id_type=MESH,
        )

    mine = pl.ds(aligned(me * cols, LANES), cols)

    def share_stream(layer, c, wide):
        s_share(2 * layer, c, jnp.sum(wide * wide, axis=1, keepdims=True), 0.0)
        gain = norm_gain[pl.ds(layer, 1), mine]
        gathered[2 * layer, chunk_rows(c), mine] = (wide * gain).astype(bf16)
        x_own(2 * layer, c)

    def loop(function):
        lax.fori_loop(0, chunks, lambda i, c: (function(i), c)[1], 0)

    def inner_first(i):
        return (1 + 2 * i) % chunks

    def ends_first(i):
        return (2 * i) % chunks

    for layer in range(layers):

        @pl.when(sp == 0)
        def _():
            glu[layer, pl.ds(0, HALO), :] = jnp.zeros((HALO, cols), bf16)

        @pl.when(sp == n - 1)
        def _():
            glu[layer, pl.ds(HALO + count, HALO), :] = jnp.zeros((HALO, cols), bf16)

    for matrix in range(layers * 3):
        own_load(matrix).wait()
    taps_load.wait()
    pl.semaphore_wait(
        barrier,
        tp - 1 + groups - 1 + (sp > 0).astype(jnp.int32) + (sp < n - 1).astype(jnp.int32),
    )
    for m in range(ahead):
        send_own(m)

    loop(lambda c: share_stream(0, c, tokens[chunk_rows(c), :].astype(f32)))

    def gated(layer, low, high, i):
        c = ends_first(i)
        phase = 2 * layer
        scale = lax.rsqrt(s_total(phase, c)[:, :1] / width + 1e-06)
        block = gathered[phase, chunk_rows(c), :]
        value = jnp.dot(block, weights[3 * layer], preferred_element_type=f32) * scale
        gate = jnp.dot(block, weights[3 * layer + 1], preferred_element_type=f32) * scale
        glu[layer, pl.ds(aligned(HALO + c * rows, HALO), rows), :] = (
            value * jax.nn.sigmoid(gate)
        ).astype(bf16)

        @pl.when(jnp.logical_and(c == 0, sp > 0))
        def _():
            h_copy(layer, 1).start()

        @pl.when(jnp.logical_and(c == chunks - 1, sp < n - 1))
        def _():
            h_copy(layer, 0).start()

        weight_share(low, high, i)

    shift = HALO - half
    groups_of_8 = (kernel + shift + 7) // 8
    window = BLOCK + 8 * groups_of_8

    def convolve(layer, c):
        lane_blocks = cols // LANES

        def block(i, carry):
            base = aligned(c * rows + (i // lane_blocks) * BLOCK, BLOCK)
            lanes = pl.ds(aligned((i % lane_blocks) * LANES, LANES), LANES)
            values = glu[layer, pl.ds(base, window), lanes].astype(f32)
            total = None
            for j in range(8):
                partial = None
                for g in range(groups_of_8):
                    tap = 8 * g + j - shift
                    if tap < 0 or tap >= kernel:
                        continue
                    term = taps[layer, pl.ds(tap, 1), lanes] * values[8 * g : 8 * g + BLOCK + 8]
                    partial = term if partial is None else partial + term
                piece_j = partial[j : j + BLOCK]
                total = piece_j if total is None else total + piece_j
            conv[pl.ds(base, BLOCK), lanes] = total
            return carry

        lax.fori_loop(0, rows // BLOCK * lane_blocks, block, 0)

    def mixed(layer, low, high, i):
        c = inner_first(i)

        @pl.when(jnp.logical_and(c == 0, sp > 0))
        def _():
            h_copy(layer, 0).wait_recv()

        @pl.when(jnp.logical_and(c == chunks - 1, sp < n - 1))
        def _():
            h_copy(layer, 1).wait_recv()

        convolve(layer, c)
        whole = conv[chunk_rows(c), :]
        s_share(
            2 * layer + 1,
            c,
            jnp.sum(whole, axis=1, keepdims=True),
            jnp.sum(whole * whole, axis=1, keepdims=True),
        )
        weight_share(low, high, i)

    def activate(layer, i):
        c = inner_first(i)
        total = s_total(2 * layer + 1, c)
        mean = total[:, :1] / width
        var = total[:, 4:5] / width - mean * mean
        gain = ln_gain[pl.ds(layer, 1), :]
        moved = ln_shift[pl.ds(layer, 1), :]
        shaped = (conv[chunk_rows(c), :] - mean) * lax.rsqrt(var + 1e-05) * gain + moved
        act = shaped * jax.nn.sigmoid(shaped)
        gathered[2 * layer + 1, chunk_rows(c), mine] = act.astype(bf16)
        x_own(2 * layer + 1, c)

    def close(layer, low, high, i):
        c = inner_first(i)
        phase = 2 * layer + 1
        x_forward(phase, c)
        x_wait(phase, c)
        update = jnp.dot(
            gathered[phase, chunk_rows(c), :],
            weights[3 * layer + 2],
            preferred_element_type=f32,
        )
        source = tokens if layer == 0 else out
        stream = (source[chunk_rows(c), :].astype(f32) + update).astype(bf16)
        out[chunk_rows(c), :] = stream
        if layer + 1 < layers:
            share_stream(layer + 1, c, stream.astype(f32))
            weight_share(low, high, i)

    def arrive(layer, low, high, i):
        c = i if layer == 0 else inner_first(i)
        x_forward(2 * layer, c)
        x_wait(2 * layer, c)
        weight_share(low, high, i)

    def due(k):
        return min(k + lead, pieces * hops)

    for layer in range(layers):
        first = 3 * layer * per_matrix
        closing = first + 2 * per_matrix
        early = due(closing + per_matrix // 6)
        middle = due(closing + per_matrix // 2)
        after = due(closing + per_matrix)
        closing = due(closing)
        opening = 0 if layer == 0 else due(first + per_matrix)
        loop(functools.partial(arrive, layer, opening, closing))
        matrix_wait(3 * layer)
        matrix_wait(3 * layer + 1)
        loop(functools.partial(gated, layer, closing, early))
        loop(functools.partial(mixed, layer, early, middle))
        loop(functools.partial(activate, layer))
        weight_steps(middle, after)
        matrix_wait(3 * layer + 2)
        loop(functools.partial(close, layer, after, due(first + 4 * per_matrix)))

    def drain_weights(i, carry):
        m, block = i // n, i % n

        @pl.when(block <= sp)
        def _():
            @pl.when(sp < n - 1)
            def _():
                z_copy(0, m, sp - block, block).wait_send()

        @pl.when(block >= sp)
        def _():
            @pl.when(sp > 0)
            def _():
                z_copy(1, m, block - sp, block).wait_send()

        @pl.when(block != sp)
        def _():
            for off in range(1, groups):
                y_copy(m, block, off, grp).wait_send()

        return carry

    lax.fori_loop(0, pieces * n, drain_weights, 0)

    def drain_chunks(i, carry):
        phase, c = i // chunks, i % chunks
        for slot in range(tp - 1):
            x_copy(phase, c, me, slot, partner).wait_send()
            s_copy(phase, c, me, slot, partner).wait_send()
        return carry

    lax.fori_loop(0, 2 * layers * chunks, drain_chunks, 0)
    for layer in range(layers):

        @pl.when(sp < n - 1)
        def _():
            h_copy(layer, 0).wait_send()

        @pl.when(sp > 0)
        def _():
            h_copy(layer, 1).wait_send()


def solution(mesh):
    groups, n, tp = mesh.shape["grp"], mesh.shape["sp"], mesh.shape["tp"]

    def shards(tokens, norm_gain, w_value, w_gate, taps, ln_gain, ln_shift, w_out):
        layers, depth, cols = w_value.shape
        count = tokens.shape[0]
        chunks = 3
        subs = 2 if depth >= 512 else 1
        ahead = 2
        pieces = layers * 3 * subs
        rows = count // chunks
        vmem = pl.BlockSpec(memory_space=pltpu.VMEM)
        hbm = pl.BlockSpec(memory_space=pl.ANY)
        dma = pltpu.SemaphoreType.DMA
        return pl.pallas_call(
            functools.partial(body, (groups, n, tp, chunks, subs, ahead)),
            out_shape=jax.ShapeDtypeStruct((count, cols), jnp.bfloat16),
            in_specs=[vmem, vmem, hbm, hbm, hbm, vmem, vmem, hbm],
            out_specs=vmem,
            scratch_shapes=[
                pltpu.VMEM(taps.shape, jnp.float32),
                pltpu.VMEM((layers * 3, depth * n, cols), jnp.bfloat16),
                pltpu.VMEM((2 * layers, count, cols * tp), jnp.bfloat16),
                pltpu.VMEM((layers, count + 2 * HALO, cols), jnp.bfloat16),
                pltpu.VMEM((count, cols), jnp.float32),
                pltpu.VMEM((2 * layers, chunks, tp, 8, rows), jnp.float32),
                dma((layers * 3 + 1,)),
                dma((2, pieces, n - 1)),
                dma((2, pieces, n - 1)),
                dma((pieces, n, groups - 1)),
                dma((pieces, n, groups - 1)),
                dma((2 * layers, chunks, tp - 1)),
                dma((2 * layers, chunks, tp)),
                dma((2 * layers, chunks, tp - 1)),
                dma((2 * layers, chunks, tp)),
                dma((layers, 2)),
                dma((layers, 2)),
            ],
            compiler_params=pltpu.CompilerParams(
                collective_id=0, has_side_effects=True, vmem_limit_bytes=60 * 1024 * 1024
            ),
        )(tokens, norm_gain, w_value, w_gate, taps, ln_gain, ln_shift, w_out)

    return jax.shard_map(
        shards,
        mesh=mesh,
        in_specs=(
            P(("grp", "sp"), "tp"),
            P(),
            P(None, "sp", "tp"),
            P(None, "sp", "tp"),
            P(None, None, "tp"),
            P(None, "tp"),
            P(None, "tp"),
            P(None, "sp", "tp"),
        ),
        out_specs=P(("grp", "sp"), "tp"),
        check_vma=False,
    )
```
